32 devices in a mesh: fs: 8 (over z, x), tp: 4 (over y, core).
Axes of the slice: x: 2, y: 2, z: 4, core: 2. Of those that a mesh axis runs over, the one named last changes fastest.
Arguments:
- tokens: bfloat16 [6144, 2048], P('fs', 'tp'), may hold values from -6 to 6
- mix_gain: float32 [2048], replicated, may hold values from 0.1 to 1.9
- outer_gate: bfloat16 [2048, 2048], P('fs', 'tp'), may hold values from -0.125 to 0.125
- inner_gate: bfloat16 [2048, 2048], P('fs', 'tp'), may hold values from -0.125 to 0.125
- signal_in: bfloat16 [2048, 2048], P('fs', 'tp'), may hold values from -0.125 to 0.125
- mix_taps: float32 [3, 2048], P(None, 'tp'), may hold values from -3 to 3
- mix_bias: float32 [2048], P('tp'), may hold values from -3 to 3
- mix_out: bfloat16 [2048, 2048], P('tp', 'fs'), may hold values from -0.1875 to 0.1875
- ffn_gain: float32 [2048], replicated, may hold values from 0.1 to 1.9
- up_gate: bfloat16 [2048, 5632], P('fs', 'tp'), may hold values from -0.125 to 0.125
- up_value: bfloat16 [2048, 5632], P('fs', 'tp'), may hold values from -0.125 to 0.125
- ffn_taps: float32 [2, 3, 5632], P(None, None, 'tp'), may hold values from -3 to 3
- ffn_bias: float32 [2, 5632], P(None, 'tp'), may hold values from -3 to 3
- down_proj: bfloat16 [5632, 2048], P('tp', 'fs'), may hold values from -0.109375 to 0.109375
Outputs:
- layer_out: bfloat16 [6144, 2048], P('fs', 'tp')
The draws below stay inside these ranges and needn't reach their ends.
All inputs are finite; a program needn't handle non-finite values.
Results may differ from the reference program's by a relative error of at most 0.023.
Values may be sent and summed in bfloat16 or wider, within the bound.
A program may use at most 64 MiB of HBM per device.

```python
import jax
import jax.numpy as jnp
from jax import lax

D = 2048
W = 2048
FF = 5632
SEQLEN = 768
TOKENS = 6144
N_FS = 8
N_TP = 4


def with_spikes(array, key, source, target, shards_of, factor):
    owner, partner = [(jnp.arange(array.shape[position]) // (array.shape[position] // shards_of)).reshape([-1 if axis == position else 1 for axis in range(array.ndim)]) for position in (source, target)]
    chosen = jax.random.permutation(key, shards_of)[partner]
    strong = (owner == chosen) | (owner == (partner + shards_of // 2) % shards_of)
    return jnp.where(strong, factor * array, array)


def block_levels(own_key, dims, cuts, low, high):
    level, own = 1.0, jax.random.fold_in(own_key, 6)
    for dim, shards_of in cuts:
        heights = jnp.exp(jax.random.uniform(jax.random.fold_in(own, dim), (shards_of,), jnp.float32, low / len(cuts), high / len(cuts)))
        level = level * jnp.repeat(heights, dims[dim] // shards_of).reshape([-1 if axis == dim else 1 for axis in range(len(dims))])
    return level


def normal_values(own_key, shape, scale, bound, cuts=(), held_as=jnp.bfloat16):
    entries = scale * jax.random.normal(own_key, shape, jnp.float32)
    if cuts:
        entries = entries * block_levels(own_key, shape, cuts, -0.22, 0.18)
    return jnp.clip(entries, -bound, bound).astype(held_as)


def heavy_noise(rng, shape, deviation, bound, cuts, heavy, held_as=jnp.bfloat16):
    values = deviation * jax.random.normal(rng, shape, jnp.float32)
    if cuts:
        values = values * block_levels(rng, shape, cuts, -0.22, 0.18)
    return jnp.clip(with_spikes(values, jax.random.fold_in(rng, 3), *heavy), -bound, bound).astype(held_as)


def setup_inputs(seed: int = 0) -> dict:
    key_of = jax.random.split(jax.random.key(seed), 15)
    tokens = normal_values(key_of[0], (TOKENS, D), 1.0, 6.0, ((0, 8), (1, 4)))
    mix_gain = jnp.clip(1.0 + 0.18 * jax.random.normal(key_of[1], (D,), jnp.float32), 0.1, 1.9)
    outer_gate = normal_values(key_of[2], (D, W), D ** -0.5, 0.125, ((0, 8), (1, 4)))
    inner_gate = normal_values(key_of[3], (D, W), D ** -0.5, 0.125, ((0, 8), (1, 4)))
    signal_in = normal_values(key_of[4], (D, W), D ** -0.5, 0.125, ((0, 8), (1, 4)))
    mix_taps = normal_values(key_of[5], (3, W), 0.577, 3.0, ((1, 4),), jnp.float32)
    mix_bias = normal_values(key_of[6], (W,), 0.5, 3.0, ((0, 4),), jnp.float32)
    mix_out = heavy_noise(key_of[7], (W, D), W ** -0.5, 0.1875, ((0, 4), (1, 8)), (0, 1, 8, 2.0))
    ffn_gain = jnp.clip(1.0 + 0.18 * jax.random.normal(key_of[8], (D,), jnp.float32), 0.1, 1.9)
    up_gate = normal_values(key_of[9], (D, FF), D ** -0.5, 0.125, ((0, 8), (1, 4)))
    up_value = normal_values(key_of[10], (D, FF), D ** -0.5, 0.125, ((0, 8), (1, 4)))
    ffn_taps = normal_values(key_of[11], (2, 3, FF), 0.577, 3.0, ((2, 4),), jnp.float32)
    ffn_bias = normal_values(key_of[12], (2, FF), 0.5, 3.0, ((1, 4),), jnp.float32)
    down_proj = heavy_noise(key_of[13], (FF, D), FF ** -0.5, 0.109375, ((0, 4), (1, 8)), (0, 1, 8, 2.0))
    return {"tokens": tokens, "mix_gain": mix_gain, "outer_gate": outer_gate, "inner_gate": inner_gate, "signal_in": signal_in, "mix_taps": mix_taps, "mix_bias": mix_bias, "mix_out": mix_out, "ffn_gain": ffn_gain, "up_gate": up_gate, "up_value": up_value, "ffn_taps": ffn_taps, "ffn_bias": ffn_bias, "down_proj": down_proj}


EPS = 1e-06

def rms_rows(values, gain):
    floats = values.astype(jnp.float32)
    scaled = floats * lax.rsqrt(lax.optimization_barrier(jnp.mean(floats * floats, axis=-1, keepdims=True)) + EPS) * gain
    return scaled.astype(jnp.bfloat16)

def causal_taps(signal, taps, bias):
    shaped = signal.reshape(N_FS, SEQLEN, signal.shape[-1])
    first = jnp.pad(shaped, ((0, 0), (1, 0), (0, 0)))[:, :-1]
    second = jnp.pad(shaped, ((0, 0), (2, 0), (0, 0)))[:, :-2]
    result = taps[2] * shaped + taps[1] * first + taps[0] * second + bias
    return result.reshape(signal.shape)

def group_sum(active, weight):
    width = active.shape[1] // N_TP
    total = jnp.zeros((active.shape[0], weight.shape[1]), jnp.float32)
    for group in range(N_TP):
        term = jnp.dot(active[:, group * width:(group + 1) * width], weight[group * width:(group + 1) * width], preferred_element_type=jnp.float32)
        total = total + lax.optimization_barrier(term.astype(jnp.bfloat16)).astype(jnp.float32)
    return total

def reference(tokens, mix_gain, outer_gate, inner_gate, signal_in, mix_taps, mix_bias, mix_out, ffn_gain, up_gate, up_value, ffn_taps, ffn_bias, down_proj):
    normed = rms_rows(tokens, mix_gain)
    outer = jnp.dot(normed, outer_gate, preferred_element_type=jnp.float32).astype(jnp.bfloat16)
    inner = jnp.dot(normed, inner_gate, preferred_element_type=jnp.float32).astype(jnp.bfloat16)
    signal = jnp.dot(normed, signal_in, preferred_element_type=jnp.float32).astype(jnp.bfloat16)
    mixed_in = inner.astype(jnp.float32) * signal.astype(jnp.float32)
    gated = (outer.astype(jnp.float32) * causal_taps(mixed_in, mix_taps, mix_bias)).astype(jnp.bfloat16)
    mixed = group_sum(gated, mix_out)
    hidden_state = (tokens.astype(jnp.float32) + mixed).astype(jnp.bfloat16)
    normed_two = rms_rows(hidden_state, ffn_gain)
    gate_pre = jnp.dot(normed_two, up_gate, preferred_element_type=jnp.float32).astype(jnp.bfloat16)
    value_pre = jnp.dot(normed_two, up_value, preferred_element_type=jnp.float32).astype(jnp.bfloat16)
    gate_conv = causal_taps(gate_pre.astype(jnp.float32), ffn_taps[0], ffn_bias[0])
    value_conv = causal_taps(value_pre.astype(jnp.float32), ffn_taps[1], ffn_bias[1])
    active = (jax.nn.silu(gate_conv) * value_conv).astype(jnp.bfloat16)
    fed = group_sum(active, down_proj)
    return (hidden_state.astype(jnp.float32) + fed).astype(jnp.bfloat16)
```

```python
import functools

import jax
import jax.numpy as jnp
from jax import lax
from jax.experimental import pallas as pl
from jax.experimental.pallas import tpu as pltpu
from jax.sharding import PartitionSpec as P

EPS = 1e-06
F32, BF16 = jnp.float32, jnp.bfloat16
MESH = pl.DeviceIdType.MESH
UP, DOWN, RIGHT, LEFT = range(4)


def grid_of(n_fs):
    nx = 1
    while nx * nx * 4 <= n_fs:
        nx *= 2
    return n_fs // nx, nx


def tiles(extent, width, body):
    whole = extent // width
    if whole:
        @pl.loop(0, whole)
        def _(i):
            body(pl.multiple_of(i * width, width), width)
    if extent % width:
        body(whole * width, extent % width)


def causal(v, taps, bias):
    row = lax.broadcasted_iota(jnp.int32, v.shape, 0)
    first = jnp.where(row < 1, 0.0, pltpu.roll(v, 1, axis=0))
    second = jnp.where(row < 2, 0.0, pltpu.roll(v, 2, axis=0))
    return taps[2] * v + taps[1] * first + taps[0] * second + bias


def kernel(
    n_fs, n_tp, tok_in, og, ig, si, mo, ug, uv, dp,
    mix_gain, ffn_gain, mix_taps, mix_bias, ffn_taps, ffn_bias,
    out,
    w0, w1, w2, w3, w4, w5, w6,
    tok, normed, state, outer, inner, signal, gate, value,
    part1, rs1, part2, rs2,
    load_sem, send_sem, recv_sem,
    tok_send, tok_recv, st_send, st_recv, p1_send, p1_recv, p2_send, p2_recv,
):
    nz, nx = grid_of(n_fs)
    fs, tp = lax.axis_index("fs"), lax.axis_index("tp")
    z, x = fs // nx, fs % nx
    bufs = (w0, w1, w2, w3, w4, w5, w6)
    sources = (og, ig, si, mo, ug, uv, dp)
    rows, own = tok.shape[1], tok.shape[2]
    per = n_fs // n_tp
    wide = part1.shape[2]

    ways = (
        (z < nz - 1, fs + nx),
        (z > 0, fs - nx),
        (x < nx - 1, fs + 1),
        (x > 0, fs - 1),
    )
    barrier = pltpu.get_barrier_semaphore()
    expected = n_tp - 1
    for there, peer in ways:
        expected = expected + jnp.where(there, 1, 0)

        @pl.when(there)
        def _(peer=peer):
            pl.semaphore_signal(barrier, inc=1, device_id={"fs": peer}, device_id_type=MESH)
    peers = [(tp + r) % n_tp for r in range(1, n_tp)]
    for peer in peers:
        pl.semaphore_signal(barrier, inc=1, device_id={"tp": peer}, device_id_type=MESH)

    loads = [pltpu.make_async_copy(s, b.at[fs], load_sem.at[i]) for i, (s, b) in enumerate(zip(sources, bufs))]
    loads.append(pltpu.make_async_copy(tok_in, tok.at[tp], load_sem.at[7]))
    for c in loads:
        c.start()
    pl.semaphore_wait(barrier, expected)

    def cut(w):
        r = bufs[w].shape[1]
        a = max(16, (r * 13 // 16) // 16 * 16)
        return ((0, a), (a, r - a))

    def piece(w, k, block, way):
        start, size = cut(w)[k]
        ref = bufs[w].at[block, pl.ds(start, size)]
        return pltpu.make_async_remote_copy(
            src_ref=ref, dst_ref=ref,
            send_sem=send_sem.at[w, k, block, way], recv_sem=recv_sem.at[w, k, block],
            device_id={"fs": ways[way][1]}, device_id_type=MESH,
        )

    def arrive(w, k, block):
        piece(w, k, block, UP).wait_recv()

    def go(w, k, block, way, cond, sending):
        @pl.when(jnp.logical_and(cond, ways[way][0]))
        def _():
            c = piece(w, k, block, way)
            if sending:
                c.start()
            else:
                c.wait_send()

    yes = z >= 0

    def along_z(w, i, sending, block_ready=None):
        half = (i + 1) // 2
        off = jnp.where(i % 2 == 1, -half, half)
        z0 = z + off
        valid = jnp.logical_and(z0 >= 0, z0 < nz)
        away = off != 0

        @pl.when(valid)
        def _():
            mine = z0 * nx + x

            def both(k, block):
                go(w, k, block, UP, z0 <= z, sending)
                go(w, k, block, DOWN, z0 >= z, sending)

            if sending:
                @pl.when(away)
                def _():
                    arrive(w, 0, mine)
            both(0, mine)
            go(w, 0, mine, RIGHT, yes, sending)
            go(w, 0, mine, LEFT, yes, sending)
            for x0 in range(nx):
                block = z0 * nx + x0
                if sending:
                    @pl.when(jnp.logical_or(away, x != x0))
                    def _():
                        arrive(w, 1, block)
                level = jnp.logical_not(away)
                go(w, 1, block, RIGHT, jnp.logical_and(level, x0 <= x), sending)
                go(w, 1, block, LEFT, jnp.logical_and(level, x0 >= x), sending)
                both(1, block)
            if block_ready is not None:
                block_ready(mine)

    def along_x(w, i, sending, block_ready=None):
        half = (i + 1) // 2
        z0 = z + jnp.where(i % 2 == 1, -half, half)

        @pl.when(jnp.logical_and(z0 >= 0, z0 < nz))
        def _():
            for dist in range(1, nx):
                for sign in (-1, 1):
                    x0 = x + sign * dist

                    @pl.when(jnp.logical_and(x0 >= 0, x0 < nx))
                    def _(sign=sign, x0=x0):
                        block = z0 * nx + x0
                        if sending:
                            arrive(w, 0, block)
                        go(w, 0, block, RIGHT if sign < 0 else LEFT, yes, sending)
            if block_ready is not None:
                @pl.loop(1, nx)
                def _(j):
                    block_ready(z0 * nx + (x + j) % nx)

    steps = 2 * nz - 1

    def pump(w, lo=1, hi=None, block_ready=None):
        last = steps + 1 if hi is None else hi

        @pl.loop(lo, last)
        def _(i):
            @pl.when(i < steps)
            def _():
                along_z(w, i, True, block_ready)
            along_x(w, i - 1, True, block_ready)

    def begin(w):
        loads[w].wait()
        along_z(w, 0, True)

    def to_owner(part, rs, send, recv, block):
        owner, k = block // per, block % per
        return owner, pltpu.make_async_remote_copy(
            src_ref=part.at[block], dst_ref=rs.at[tp, k],
            send_sem=send.at[block], recv_sem=recv.at[tp, k],
            device_id={"tp": owner}, device_id_type=MESH,
        )

    def from_peer(rs, recv, src, k):
        ref = rs.at[src, k]
        pltpu.make_async_remote_copy(
            src_ref=ref, dst_ref=ref, send_sem=p1_send.at[0], recv_sem=recv.at[src, k],
            device_id={"tp": src}, device_id_type=MESH,
        ).wait_recv()

    def spread(buf, send, recv):
        return [
            pltpu.make_async_remote_copy(
                src_ref=buf.at[tp], dst_ref=buf.at[tp], send_sem=send.at[r], recv_sem=recv.at[tp],
                device_id={"tp": peer}, device_id_type=MESH,
            )
            for r, peer in enumerate(peers)
        ]

    def collect(buf, send, recv):
        for peer in peers:
            pltpu.make_async_remote_copy(
                src_ref=buf.at[peer], dst_ref=buf.at[peer], send_sem=send.at[0], recv_sem=recv.at[peer],
                device_id={"tp": peer}, device_id_type=MESH,
            ).wait_recv()

    def norm(buf, gain):
        step = 64

        @pl.loop(0, rows // step)
        def _(m):
            at = pl.ds(pl.multiple_of(m * step, step), step)
            total = jnp.zeros((step, 1), F32)
            for t in range(n_tp):
                v = buf[t, at, :].astype(F32)
                total = total + jnp.sum(v * v, axis=-1, keepdims=True)
            scale = lax.rsqrt(total / (n_tp * own) + EPS)
            for t in range(n_tp):
                cols = slice(t * own, (t + 1) * own)
                v = buf[t, at, :].astype(F32)
                normed[at, cols] = (v * scale * gain[:, cols]).astype(BF16)

    mt = 256 if rows % 256 == 0 else rows

    def project(w, dst):
        n, r, c = bufs[w].shape

        def column(start, size):
            @pl.loop(0, rows // mt)
            def _(m):
                at = pl.ds(pl.multiple_of(m * mt, mt), mt)
                weight = bufs[w][:, :, pl.ds(start, size)].reshape(n * r, size)
                dst[at, pl.ds(start, size)] = jnp.dot(
                    normed[at, :], weight, preferred_element_type=F32
                ).astype(BF16)
        tiles(c, 256, column)

    def out_block(w, act, part, rs, send, recv, block):
        @pl.loop(0, rows // mt)
        def _(m):
            at = pl.ds(pl.multiple_of(m * mt, mt), mt)
            part[block, at, :] = jnp.dot(
                act[at, :], bufs[w][block], preferred_element_type=F32
            ).astype(BF16)
        owner, c = to_owner(part, rs, send, recv, block)

        @pl.when(owner != tp)
        def _():
            c.start()

    def add_up(base, part, rs, recv, dst):
        for peer in peers:
            for k in range(per):
                from_peer(rs, recv, peer, k)
        step = 128

        @pl.loop(0, rows // step)
        def _(m):
            at = pl.ds(pl.multiple_of(m * step, step), step)
            for k in range(per):
                cols = slice(k * wide, (k + 1) * wide)
                total = part[tp * per + k, at, :].astype(F32)
                for peer in peers:
                    total = total + rs[peer, k, at, :].astype(F32)
                dst[at, cols] = (base[at, cols].astype(F32) + total).astype(BF16)

    loads[7].wait()
    begin(0)
    begin(1)
    tok_copies = spread(tok, tok_send, tok_recv)
    for c in tok_copies:
        c.start()
    pump(0)
    begin(2)
    pump(1)
    begin(3)
    collect(tok, tok_send, tok_recv)
    norm(tok, mix_gain)
    pump(2, 1, 4)
    project(0, outer)
    pump(2, 4)
    begin(4)
    project(1, inner)
    pump(3, 1, 4)
    project(2, signal)

    def mixer(start, size):
        cols = pl.ds(start, size)
        taps = [mix_taps[j:j + 1, cols] for j in range(3)]
        v = inner[:, cols].astype(F32) * signal[:, cols].astype(F32)
        outer[:, cols] = (outer[:, cols].astype(F32) * causal(v, taps, mix_bias[:, cols])).astype(BF16)
    tiles(outer.shape[1], 128, mixer)
    pump(3, 4)
    begin(5)

    @pl.loop(0, n_fs)
    def _(block):
        out_block(3, outer, part1, rs1, p1_send, p1_recv, block)
    pump(4, 1, 4)
    add_up(tok.at[tp], part1, rs1, p1_recv, state.at[tp])
    st_copies = spread(state, st_send, st_recv)
    for c in st_copies:
        c.start()
    pump(4, 4)
    begin(6)
    pump(5, 1, 4)
    collect(state, st_send, st_recv)
    norm(state, ffn_gain)
    project(4, gate)
    pump(5, 4)

    pump(6, 1, 3)
    project(5, value)

    def feed(start, size):
        cols = pl.ds(start, size)
        g = causal(gate[:, cols].astype(F32), [ffn_taps[j:j + 1, cols] for j in range(3)], ffn_bias[0:1, cols])
        v = causal(value[:, cols].astype(F32), [ffn_taps[j:j + 1, cols] for j in range(3, 6)], ffn_bias[1:2, cols])
        gate[:, cols] = (g / (1.0 + jnp.exp(-g)) * v).astype(BF16)
    tiles(gate.shape[1], 128, feed)

    @pl.loop(0, steps + 1)
    def _(i):
        def block_out(block):
            out_block(6, gate, part2, rs2, p2_send, p2_recv, block)

        half = (i + 1) // 2
        z0 = z + jnp.where(i % 2 == 1, -half, half)
        before = i // 2
        z1 = z + jnp.where(i % 2 == 0, -before, before)

        @pl.when(jnp.logical_and(i >= 3, i < steps))
        def _():
            along_z(6, i, True)

        @pl.when(i >= 3)
        def _():
            along_x(6, i - 1, True)

        @pl.loop(0, nx)
        def _(j):
            z_of = jnp.where(j == 0, z0, z1)
            good = jnp.logical_and(z_of >= 0, z_of < nz)
            good = jnp.logical_and(good, jnp.where(j == 0, i < steps, i >= 1))

            @pl.when(good)
            def _():
                block_out(z_of * nx + (x + j) % nx)

    add_up(state.at[tp], part2, rs2, p2_recv, out)

    for c in tok_copies + st_copies:
        c.wait_send()
    for part, rs, send, recv in ((part1, rs1, p1_send, p1_recv), (part2, rs2, p2_send, p2_recv)):
        @pl.loop(0, n_fs)
        def _(block):
            owner, c = to_owner(part, rs, send, recv, block)

            @pl.when(owner != tp)
            def _():
                c.wait_send()
    for w in range(7):
        @pl.loop(0, steps)
        def _(i):
            along_z(w, i, False)
            along_x(w, i, False)


def solution(mesh):
    n_fs, n_tp = mesh.shape["fs"], mesh.shape["tp"]

    def on_device(
        tokens, mix_gain, outer_gate, inner_gate, signal_in, mix_taps, mix_bias, mix_out,
        ffn_gain, up_gate, up_value, ffn_taps, ffn_bias, down_proj,
    ):
        rows, own = tokens.shape
        weights = (outer_gate, inner_gate, signal_in, mix_out, up_gate, up_value, down_proj)
        chan, hidden = outer_gate.shape[1], up_gate.shape[1]
        wide = mix_out.shape[1]
        model = own * n_tp
        hbm = pl.BlockSpec(memory_space=pl.ANY)
        vmem = pl.BlockSpec(memory_space=pltpu.VMEM)
        dma = pltpu.SemaphoreType.DMA
        per = n_fs // n_tp
        return pl.pallas_call(
            functools.partial(kernel, n_fs, n_tp),
            out_shape=jax.ShapeDtypeStruct(tokens.shape, BF16),
            in_specs=[hbm] * 8 + [vmem] * 6,
            out_specs=vmem,
            scratch_shapes=[pltpu.VMEM((n_fs, *w.shape), BF16) for w in weights]
            + [
                pltpu.VMEM((n_tp, rows, own), BF16),
                pltpu.VMEM((rows, model), BF16),
                pltpu.VMEM((n_tp, rows, own), BF16),
                pltpu.VMEM((rows, chan), BF16),
                pltpu.VMEM((rows, chan), BF16),
                pltpu.VMEM((rows, chan), BF16),
                pltpu.VMEM((rows, hidden), BF16),
                pltpu.VMEM((rows, hidden), BF16),
                pltpu.VMEM((n_fs, rows, wide), BF16),
                pltpu.VMEM((n_tp, per, rows, wide), BF16),
                pltpu.VMEM((n_fs, rows, wide), BF16),
                pltpu.VMEM((n_tp, per, rows, wide), BF16),
                dma((8,)),
                dma((7, 2, n_fs, 4)),
                dma((7, 2, n_fs)),
                dma((n_tp,)), dma((n_tp,)),
                dma((n_tp,)), dma((n_tp,)),
                dma((n_fs,)), dma((n_tp, per)),
                dma((n_fs,)), dma((n_tp, per)),
            ],
            compiler_params=pltpu.CompilerParams(
                collective_id=0, has_side_effects=True, vmem_limit_bytes=67043328
            ),
        )(
            tokens, *weights, mix_gain[None], ffn_gain[None], mix_taps, mix_bias[None],
            ffn_taps.reshape(6, hidden), ffn_bias,
        )

    return jax.shard_map(
        on_device,
        mesh=mesh,
        in_specs=(
            P("fs", "tp"), P(), P("fs", "tp"), P("fs", "tp"), P("fs", "tp"), P(None, "tp"), P("tp"),
            P("tp", "fs"), P(), P("fs", "tp"), P("fs", "tp"), P(None, None, "tp"), P(None, "tp"),
            P("tp", "fs"),
        ),
        out_specs=P("fs", "tp"),
        check_vma=False,
    )
```
